1024 devices in a mesh: grp: 2 (over x), fs: 16 (over z), tp: 32 (over y, core).
Axes of the slice: x: 2, y: 16, z: 16, core: 2. Of those that a mesh axis runs over, the one named last changes fastest.
The devices are a block of a 4x16x16 slice.
Arguments:
- tokens: bfloat16 [7680, 2048], P(('grp', 'tp')), parts along dimension 0, may hold values from -60 to 60
- route_expert: int32 [7680, 4], P(('grp', 'tp')), parts along dimension 0, may hold values from 0 to 31, all different within a row; in each aligned block of 120 rows (0 to 119, 120 to 239, ...) at most 16 rows name the same one
- route_weight: float32 [7680, 4], P(('grp', 'tp')), parts along dimension 0, may hold values from 0.05 to 1
- norm_gain: float32 [2048], P('tp'), may hold values from 0.1 to 1.9
- gate_train: float32 [32, 2048, 2048], P(None, 'tp', 'fs'), may hold values from -8 to 8
- up_train: float32 [32, 2048, 2048], P(None, 'tp', 'fs'), may hold values from -8 to 8
- down_train: float32 [32, 2048, 2048], P(None, 'tp', 'fs'), may hold values from -0.013671875 to 0.013671875
Outputs:
- gate_serve: bfloat16 [64, 2048, 2048], P(('grp', 'tp'), None, 'fs'), parts along dimension 0
- up_serve: bfloat16 [64, 2048, 2048], P(('grp', 'tp'), None, 'fs'), parts along dimension 0
- down_serve: bfloat16 [64, 2048, 2048], P(('grp', 'tp'), None, 'fs'), parts along dimension 0
- mixed: bfloat16 [7680, 2048], P(('grp', 'tp'), 'fs'), parts along dimension 0
The draws below stay inside these ranges and needn't reach their ends.
There are 2 independent parts, one for each index of `grp`. The reference program is written for one: setup_inputs(seed, part) draws one part's arguments, and reference() takes and returns one part's arrays. A program takes and returns all parts, laid end to end along the dimension named above; an argument that names none is the same for every part. Nothing has to cross between parts.
Inputs may be any that keep to these rules, and one draw needn't show every extreme that they name: `route_expert`: each row names 4 different experts; the rows of one device name each expert at most 16 times.
All inputs are finite; a program needn't handle non-finite values.
Results may differ from the reference program's by a relative error of at most 0.0087.
Values may be sent and summed in bfloat16 or wider, within the bound.
No kernel may reach another device: no remote copies, remote signals or barrier semaphores. Data moves between devices by JAX's collectives and lax.ppermute only.
A program may use at most 32 MiB of HBM per device.

```python
import math
import jax
import jax.numpy as jnp
import numpy as np
from jax import lax

D = 2048
FF = 2048
EXPERTS = 32
TOP = 4
TOK_DEV = 120
CAP = 16
TOKENS = 3840
N_TP = 32


def draw_tokens(key, part):
    keys = jax.random.split(jax.random.fold_in(key, 11), 3)
    row_scale = jnp.exp(jax.random.uniform(keys[0], (TOKENS, 1), jnp.float32, math.log(0.3), math.log(3.0)))
    col_scale = jnp.exp(jax.random.uniform(keys[1], (1, D), jnp.float32, math.log(0.3), math.log(3.0)))
    base = jnp.clip(jax.random.normal(keys[2], (TOKENS, D), jnp.float32), -6.0, 6.0)
    return (base * row_scale * col_scale).astype(jnp.bfloat16)


def weight_columns(key, salt):
    keys = jax.random.split(jax.random.fold_in(key, salt), 2)
    scales = jnp.exp(jax.random.uniform(keys[0], (EXPERTS, 1, FF), jnp.float32, math.log(0.5), math.log(8.0)))
    base = jnp.clip(jax.random.normal(keys[1], (EXPERTS, D, FF), jnp.float32), -6.0, 6.0)
    return (base * scales * D ** (-0.5)).astype(jnp.float32)


def draw_gate_train(key, part):
    return weight_columns(key, 21)


def draw_up_train(key, part):
    return weight_columns(key, 22)


def level_of(rng, shape, cuts, low, high):
    def one(dim, parts):
        steps = jax.random.uniform(jax.random.fold_in(jax.random.fold_in(rng, 6), dim), (parts,), jnp.float32, low / len(cuts), high / len(cuts))
        return jnp.repeat(jnp.exp(steps), shape[dim] // parts).reshape((-1,) + (1,) * (len(shape) - dim - 1))

    level = one(*cuts[0])
    for cut in cuts[1:]:
        level = level * one(*cut)
    return level


def deal_out(rng, own, number, rows, number_of, top, reach, lean):
    order = jax.random.permutation(rng, number_of)
    crowded, usual = portions_of(number_of, rows * top, reach, lean, True), portions_of(number_of, rows * top, reach, lean, False)
    places = jnp.arange(number_of)

    def named(sizes, offset_by):
        used = int((sizes > 0).sum())
        fixed = max(1, used // 4)
        shifted = fixed + (places - fixed + offset_by * (used - fixed)) % max(1, number_of - fixed)
        return jnp.zeros((number_of,), jnp.int32).at[order[jnp.where(places < fixed, places, shifted)]].set(jnp.asarray(sizes, jnp.int32))

    sizes = jnp.where(number % 4 == 0, named(crowded, number // 4), named(usual, number - number // 4 - 1))
    mixed = jax.random.permutation(jax.random.fold_in(own, 3), number_of)
    giver, sink = mixed[0:number_of // 2 * 2:2], mixed[1:number_of // 2 * 2:2]
    margin = jnp.minimum(sizes[giver] - 1, reach - sizes[sink]) // 2
    margin = jnp.where((giver == order[0]) | (sink == order[0]) | (sizes[sink] == 0), 0, jnp.maximum(margin, 0))
    shifted = jax.random.randint(jax.random.fold_in(own, 4), (number_of // 2,), 0, 1 << 20) % (margin + 1)
    sizes = sizes.at[giver].add(-shifted).at[sink].add(shifted)
    labels = jnp.searchsorted(jnp.cumsum(sizes), jnp.arange(rows * top), side="right").astype(jnp.int32)
    listing = labels.reshape(top, rows).T
    listing = listing[jax.random.permutation(jax.random.fold_in(own, 1), rows)]
    offset_by = jax.random.randint(jax.random.fold_in(own, 2), (rows, 1), 0, top)
    return jnp.take_along_axis(listing, (jnp.arange(top)[None, :] + offset_by) % top, axis=1)


def portions_of(count, total, reach, slope, full):
    portions = [(1 << 20) // math.isqrt(grade ** slope) + 1 for grade in range(1, count + 1)]
    largest = reach if full else min(reach, max(-(-total // count), total * portions[0] // sum(portions)))
    least = 1 if total - largest >= count - 1 else 0
    given, surplus = [largest] + [least] * (count - 1), total - largest - least * (count - 1)
    while surplus > 0:
        movable = [i for i in range(1, count) if given[i] < largest] or [i for i in range(1, count) if given[i] < reach]
        pool, left = sum([portions[i] for i in movable]), surplus
        for i in movable:
            extra = min(reach - given[i], max(1, left * portions[i] // pool), surplus)
            given[i] = given[i] + extra
            surplus = surplus - extra
    return np.array(given)


def noise(own_key, extent, deviation, reach, cuts=(), kind=jnp.bfloat16):
    values = jax.random.normal(own_key, extent, jnp.float32) * deviation
    if len(cuts) > 0:
        values = level_of(own_key, extent, cuts, -0.22, 0.18) * values
    return jnp.clip(values, min=-reach, max=reach).astype(kind)


def setup_inputs(seed: int = 0, part: int = 0) -> dict:
    key_list = jax.random.split(jax.random.key(seed), 8)
    part_splits = jax.random.split(jax.random.fold_in(key_list[7], part), 8)
    tokens = draw_tokens(jax.random.fold_in(jax.random.fold_in(key_list[7], part), 71), part)
    route_expert_keys = jax.random.split(jax.random.fold_in(part_splits[1], 1), TOKENS // TOK_DEV)
    route_expert_turns = jax.random.permutation(jax.random.fold_in(part_splits[1], 3), TOKENS // TOK_DEV)
    route_expert = jax.vmap(lambda own, number: deal_out(jax.random.fold_in(part_splits[1], 2), own, number, TOK_DEV, EXPERTS, TOP, CAP, 2))(route_expert_keys, route_expert_turns).reshape((TOKENS, TOP))
    route_weight = jnp.clip(jnp.exp(math.log(1.0) - 2.9957323 * jax.random.uniform(part_splits[2], (TOKENS, TOP), jnp.float32) ** level_of(part_splits[2], (TOKENS, TOP), ((0, 32),), -0.2, 0.2)), 0.05, 1.0)
    norm_gain = jnp.clip(1.0 + 0.18 * jax.random.normal(key_list[3], (D,), jnp.float32), 0.1, 1.9)
    gate_train = draw_gate_train(jax.random.fold_in(key_list[7], 71), part)
    up_train = draw_up_train(jax.random.fold_in(key_list[7], 71), part)
    down_train = noise(key_list[6], (EXPERTS, FF, D), (FF * 100) ** -0.5, 0.013671875, ((1, 32), (2, 16)), jnp.float32)
    return dict(tokens=tokens, route_expert=route_expert, route_weight=route_weight, norm_gain=norm_gain, gate_train=gate_train, up_train=up_train, down_train=down_train)


def activate(gate_pre, up_pre):
    clamped = jnp.minimum(gate_pre, 7.0)
    bounded = jnp.clip(up_pre, -7.0, 7.0)
    return (clamped * jax.nn.sigmoid(1.702 * clamped) * (bounded + 1.0)).astype(jnp.bfloat16)

def reference(tokens, route_expert, route_weight, norm_gain, gate_train, up_train, down_train):
    gate_serve = (gate_train * norm_gain[None, :, None]).astype(jnp.bfloat16)
    up_serve = (up_train * norm_gain[None, :, None]).astype(jnp.bfloat16)
    down_serve = down_train.astype(jnp.bfloat16)
    floated = tokens.astype(jnp.float32)
    normed = (floated * lax.rsqrt(lax.optimization_barrier(jnp.mean(floated * floated, axis=-1, keepdims=True)) + 1e-06)).astype(jnp.bfloat16)
    flat_expert = route_expert.reshape(-1).astype(jnp.int32)
    expert_ids = jnp.arange(EXPERTS, dtype=jnp.int32)
    onehot = (flat_expert[:, None] == expert_ids[None, :]).astype(jnp.int32)
    slot_rank = lax.optimization_barrier(jnp.sum((jnp.cumsum(onehot, axis=0) - 1) * onehot, axis=1)).astype(jnp.int32)
    flat_token = (jnp.arange(TOKENS * TOP, dtype=jnp.int32) // TOP).astype(jnp.int32)
    row_table = jnp.full((EXPERTS, N_TP * CAP), TOKENS, jnp.int32).at[flat_expert, slot_rank].set(flat_token)
    padded = jnp.concatenate([normed, jnp.zeros((1, D), jnp.bfloat16)], axis=0)

    def one_expert(inputs):
        row_ids, gate_one, up_one, down_one = inputs
        gathered = padded[row_ids]
        gate_pre = jnp.dot(gathered, gate_one, preferred_element_type=jnp.float32)
        up_pre = jnp.dot(gathered, up_one, preferred_element_type=jnp.float32)
        hidden = activate(gate_pre, up_pre)
        return jnp.dot(hidden, down_one, preferred_element_type=jnp.float32).astype(jnp.bfloat16)
    expert_rows = lax.map(one_expert, (row_table, gate_serve, up_serve, down_serve))
    picked = expert_rows[flat_expert, slot_rank].reshape(TOKENS, TOP, D)
    mixed = lax.optimization_barrier(jnp.sum(route_weight[:, :, None] * picked.astype(jnp.float32), axis=1)).astype(jnp.bfloat16)
    return (gate_serve, up_serve, down_serve, mixed)
```

```python
import functools

import jax
import jax.numpy as jnp
from jax import lax
from jax.experimental import pallas as pl
from jax.experimental.pallas import tpu as pltpu
from jax.sharding import PartitionSpec as P


EXPERTS = 32
TOP = 4
CAP = 16
SUB = 4
F32 = jnp.float32
BF16 = jnp.bfloat16


def vm():
    return pl.BlockSpec(memory_space=pltpu.VMEM)


def sm():
    return pl.BlockSpec(memory_space=pltpu.SMEM)


def prep_kernel(block, tokens, route_t, weight_t, buffer, comb_hi, comb_lo):
    rows, _ = tokens.shape
    floated = tokens[...].astype(F32)
    inv = lax.rsqrt(jnp.mean(floated * floated, axis=-1, keepdims=True) + 1e-06)
    cols = buffer.shape[1]
    part = tokens[:, pl.ds(pl.multiple_of(block[0] * cols, cols), cols)].astype(F32)
    normed = (part * inv).astype(BF16)
    expert = lax.broadcasted_iota(jnp.int32, (EXPERTS, rows), 0)
    named = jnp.zeros((EXPERTS, rows), F32)
    weight = jnp.zeros((EXPERTS, rows), F32)
    for k in range(TOP):
        hit = route_t[k : k + 1, :] == expert
        named = named + jnp.where(hit, 1.0, 0.0)
        weight = weight + jnp.where(hit, weight_t[k : k + 1, :], 0.0)
    earlier = lax.broadcasted_iota(jnp.int32, (rows, rows), 0) < lax.broadcasted_iota(
        jnp.int32, (rows, rows), 1
    )
    rank = jnp.dot(
        named.astype(BF16),
        jnp.where(earlier, 1.0, 0.0).astype(BF16),
        preferred_element_type=F32,
    )
    rank = jnp.where(named > 0.5, rank, -1.0)
    slot = lax.broadcasted_iota(jnp.int32, (EXPERTS, CAP, rows), 1).astype(F32)
    taken = rank[:, None, :] == slot
    scatter = jnp.where(taken, 1.0, 0.0).reshape(EXPERTS * CAP, rows)
    buffer[...] = jnp.dot(scatter.astype(BF16), normed, preferred_element_type=F32).astype(BF16)
    comb = jnp.where(taken, weight[:, None, :], 0.0).reshape(EXPERTS * CAP, rows)
    high = comb.astype(BF16)
    comb_hi[...] = high
    comb_lo[...] = (comb - high.astype(F32)).astype(BF16)


def pieces(own, below, above, below2, above2, res, stride):
    half = SUB // 2
    out = []
    for ref, r in ((own, res), (below, (res + stride - 1) % stride), (above, (res + 1) % stride)):
        for k in range(0, SUB, 2):
            out.append((ref, k, k, r))
    for k in range(0, half, 2):
        out.append((below2, k, k, (res + 2) % stride))
        out.append((above2, k, half + k, (res + 2) % stride))
    return out


def passed_on(pairs, sems):
    return [pltpu.make_async_copy(src, dst, sems.at[i]) for i, (src, dst) in enumerate(pairs)]


def block_of(w, k, r, stride, at, size):
    per = w.shape[0] // (SUB * stride)
    first = (k * stride + r) * per
    return jnp.concatenate([w[first + j, at : at + size, :] for j in range(per)], axis=0)


def gate_up_kernel(
    res, own, below, above, below2, above2, weight, hidden, gate_out, up_out, rhs, sems, *, stride
):
    rows, width = hidden.shape
    size = weight.shape[1] // 2
    copies = passed_on(
        ((weight.at[:, :size, :], gate_out), (weight.at[:, size:, :], up_out)), sems
    )
    for c in copies:
        c.start()
    order = pieces(own, below, above, below2, above2, res[0], stride)
    for n, (_, _, wk, r) in enumerate(order):
        for j in range(2):
            half = rhs.at[n, j * (rhs.shape[1] // 2) : (j + 1) * (rhs.shape[1] // 2), :]
            half[:, :width] = block_of(weight, wk + j, r, stride, 0, size)
            half[:, width:] = block_of(weight, wk + j, r, stride, size, size)
    step = 128

    def one(i, carry):
        at = pl.ds(pl.multiple_of(i * step, step), step)
        acc = jnp.zeros((step, 2 * width), F32)
        for n, (ref, k, _, _) in enumerate(order):
            lhs = jnp.concatenate([ref[k, at, :], ref[k + 1, at, :]], axis=1)
            acc = acc + jnp.dot(lhs, rhs[n], preferred_element_type=F32)
        g = jnp.minimum(acc[:, :width], 7.0)
        u = jnp.clip(acc[:, width:], -7.0, 7.0)
        hidden[at, :] = (g * jax.nn.sigmoid(1.702 * g) * (u + 1.0)).astype(BF16)
        return carry

    lax.fori_loop(0, rows // step, one, 0)
    for c in copies:
        c.wait()


def down_kernel(
    res, own, below, above, below2, above2, weight, out, down_out, rhs, sems, *, stride
):
    rows, width = out.shape
    copies = passed_on(((weight, down_out),), sems)
    for c in copies:
        c.start()
    order = pieces(own, below, above, below2, above2, res[0], stride)
    for n, (_, _, wk, r) in enumerate(order):
        for j in range(2):
            half = rhs.at[n, j * (rhs.shape[1] // 2) : (j + 1) * (rhs.shape[1] // 2), :]
            half[...] = block_of(weight, wk + j, r, stride, 0, weight.shape[1])
    step = 128

    def one(i, carry):
        at = pl.ds(pl.multiple_of(i * step, step), step)
        acc = jnp.zeros((step, width), F32)
        for n, (ref, k, _, _) in enumerate(order):
            lhs = jnp.concatenate([ref[k, at, :], ref[k + 1, at, :]], axis=1)
            acc = acc + jnp.dot(lhs, rhs[n], preferred_element_type=F32)
        out[at, :] = acc.astype(BF16)
        return carry

    lax.fori_loop(0, rows // step, one, 0)
    for c in copies:
        c.wait()


def combine_kernel(comb_hi, comb_lo, rows, mixed):
    dims = (((0,), (0,)), ((), ()))
    acc = lax.dot_general(comb_hi[...], rows[...], dims, preferred_element_type=F32)
    acc = acc + lax.dot_general(comb_lo[...], rows[...], dims, preferred_element_type=F32)
    mixed[...] = acc.astype(BF16)


def exchange(x):
    return lax.all_to_all(x, "tp", split_axis=0, concat_axis=0, tiled=True)


def after(x, *others):
    return lax.optimization_barrier((x, *others))[0]


def gather(block):
    count = lax.axis_size("fs")
    stride = count // SUB
    groups = [[i + stride * j for j in range(SUB)] for i in range(stride)]
    own = lax.all_gather(block, "fs", axis=0, axis_index_groups=groups)

    def shift(x, by):
        return lax.ppermute(x, "fs", [(i, (i + by) % count) for i in range(count)])

    half = SUB // 2
    return (
        own,
        shift(own, 1),
        shift(own, -1),
        shift(own[:half], 2),
        shift(own[half:], -2),
    )


def body(tokens, route_expert, route_weight, norm_gain, gate_train, up_train, down_train):
    tp_count = lax.axis_size("tp")
    fs_count = lax.axis_size("fs")
    stride = fs_count // SUB
    tok_rows, width = tokens.shape
    cols = width // fs_count
    slots = EXPERTS * CAP
    my_block = lax.axis_index("fs").astype(jnp.int32)
    res = (my_block % stride).reshape(1)

    buffer, comb_hi, comb_lo = pl.pallas_call(
        prep_kernel,
        in_specs=[sm(), vm(), vm(), vm()],
        out_specs=[vm(), vm(), vm()],
        out_shape=[
            jax.ShapeDtypeStruct((slots, cols), BF16),
            jax.ShapeDtypeStruct((slots, tok_rows), BF16),
            jax.ShapeDtypeStruct((slots, tok_rows), BF16),
        ],
        name="prep",
    )(my_block.reshape(1), tokens, route_expert.T, route_weight.T)
    arrived = exchange(buffer.reshape(EXPERTS, CAP, cols)).reshape(slots, cols)

    gain = norm_gain[None, :, None]
    packed = jnp.concatenate(
        [(gate_train * gain).astype(BF16), (up_train * gain).astype(BF16)], axis=1
    )
    both = exchange(after(packed, arrived))
    served = jax.ShapeDtypeStruct(down_train.shape, BF16)
    hbm = pl.BlockSpec(memory_space=pl.ANY)
    pairs = fs_count // 2

    hidden, gate_serve, up_serve = pl.pallas_call(
        functools.partial(gate_up_kernel, stride=stride),
        in_specs=[sm()] + [vm()] * 6,
        out_specs=[vm(), hbm, hbm],
        out_shape=[jax.ShapeDtypeStruct((slots, both.shape[2]), BF16), served, served],
        scratch_shapes=[
            pltpu.VMEM((pairs, 2 * cols, 2 * both.shape[2]), BF16),
            pltpu.SemaphoreType.DMA((2,)),
        ],
        name="gate_up",
    )(res, *gather(arrived), both)
    arrived_down = exchange(after(down_train.astype(BF16), both))
    expert_out, down_serve = pl.pallas_call(
        functools.partial(down_kernel, stride=stride),
        in_specs=[sm()] + [vm()] * 6,
        out_specs=[vm(), hbm],
        out_shape=[jax.ShapeDtypeStruct((slots, down_train.shape[2]), BF16), served],
        scratch_shapes=[
            pltpu.VMEM((pairs, 2 * both.shape[2], down_train.shape[2]), BF16),
            pltpu.SemaphoreType.DMA((1,)),
        ],
        name="down",
    )(res, *gather(hidden), arrived_down)
    returned = exchange(expert_out.reshape(tp_count, slots // tp_count, -1)).reshape(slots, -1)
    mixed = pl.pallas_call(
        combine_kernel,
        in_specs=[vm()] * 3,
        out_specs=vm(),
        out_shape=jax.ShapeDtypeStruct((tok_rows, returned.shape[1]), BF16),
        name="combine",
    )(comb_hi, comb_lo, returned)

    def whole(w):
        return w.reshape(1, -1, w.shape[-1])

    return (whole(gate_serve), whole(up_serve), whole(down_serve), mixed)


def solution(mesh):
    return jax.shard_map(
        body,
        mesh=mesh,
        in_specs=(
            P(("grp", "tp"), None),
            P(("grp", "tp"), None),
            P(("grp", "tp"), None),
            P("tp"),
            P(None, "tp", "fs"),
            P(None, "tp", "fs"),
            P(None, "tp", "fs"),
        ),
        out_specs=(
            P(("grp", "tp"), None, "fs"),
            P(("grp", "tp"), None, "fs"),
            P(("grp", "tp"), None, "fs"),
            P(("grp", "tp"), "fs"),
        ),
        check_vma=False,
    )
```

```python
import functools

import jax
import jax.numpy as jnp
from jax import lax
from jax.experimental import pallas as pl
from jax.experimental.pallas import tpu as pltpu
from jax.sharding import PartitionSpec as P


EXPERTS = 32
TOP = 4
CAP = 16
SUB = 4
F32 = jnp.float32
BF16 = jnp.bfloat16


def vm():
    return pl.BlockSpec(memory_space=pltpu.VMEM)


def sm():
    return pl.BlockSpec(memory_space=pltpu.SMEM)


def prep_kernel(block, tokens, route_t, weight_t, buffer, comb_hi, comb_lo):
    rows, _ = tokens.shape
    floated = tokens[...].astype(F32)
    inv = lax.rsqrt(jnp.mean(floated * floated, axis=-1, keepdims=True) + 1e-06)
    cols = buffer.shape[1]
    part = tokens[:, pl.ds(pl.multiple_of(block[0] * cols, cols), cols)].astype(F32)
    normed = (part * inv).astype(BF16)
    expert = lax.broadcasted_iota(jnp.int32, (EXPERTS, rows), 0)
    named = jnp.zeros((EXPERTS, rows), F32)
    weight = jnp.zeros((EXPERTS, rows), F32)
    for k in range(TOP):
        hit = route_t[k : k + 1, :] == expert
        named = named + jnp.where(hit, 1.0, 0.0)
        weight = weight + jnp.where(hit, weight_t[k : k + 1, :], 0.0)
    earlier = lax.broadcasted_iota(jnp.int32, (rows, rows), 0) < lax.broadcasted_iota(
        jnp.int32, (rows, rows), 1
    )
    rank = jnp.dot(
        named.astype(BF16),
        jnp.where(earlier, 1.0, 0.0).astype(BF16),
        preferred_element_type=F32,
    )
    rank = jnp.where(named > 0.5, rank, -1.0)
    slot = lax.broadcasted_iota(jnp.int32, (EXPERTS, CAP, rows), 1).astype(F32)
    taken = rank[:, None, :] == slot
    scatter = jnp.where(taken, 1.0, 0.0).reshape(EXPERTS * CAP, rows)
    buffer[...] = jnp.dot(scatter.astype(BF16), normed, preferred_element_type=F32).astype(BF16)
    comb = jnp.where(taken, weight[:, None, :], 0.0).reshape(EXPERTS * CAP, rows)
    high = comb.astype(BF16)
    comb_hi[...] = high
    comb_lo[...] = (comb - high.astype(F32)).astype(BF16)


def pieces(own, below, above, below2, above2, res, stride):
    half = SUB // 2
    out = []
    for ref, r in ((own, res), (below, (res + stride - 1) % stride), (above, (res + 1) % stride)):
        for k in range(0, SUB, 2):
            out.append((ref, k, k, r))
    for k in range(0, half, 2):
        out.append((below2, k, k, (res + 2) % stride))
        out.append((above2, k, half + k, (res + 2) % stride))
    return out


def part_at(first, k, parts, size):
    return pl.ds(pl.multiple_of(((first + parts - k) % parts) * size, size), size)


def gate_up_kernel(ids, *refs, stride, parts):
    five, weights = refs[:5], refs[5 : 5 + parts]
    hidden, gate_out, up_out, whole, sems = refs[5 + parts :]
    rows, width = hidden.shape
    size = weights[0].shape[1] // 2
    copies = []
    for k, w in enumerate(weights):
        at = part_at(ids[1], k, parts, size)
        for j, dst in enumerate((gate_out, up_out)):
            src = w.at[:, j * size : (j + 1) * size, :]
            copies.append(pltpu.make_async_copy(src, dst.at[:, at, :], sems.at[2 * k + j]))
            whole[:, at, j * width : (j + 1) * width] = w[:, j * size : (j + 1) * size, :]
    for c in copies:
        c.start()
    order = pieces(*five, ids[0], stride)
    step = 128

    def one(i, carry):
        at = pl.ds(pl.multiple_of(i * step, step), step)
        acc = multiply(order, at, whole, stride)
        g = jnp.minimum(acc[:, :width], 7.0)
        u = jnp.clip(acc[:, width:], -7.0, 7.0)
        hidden[at, :] = (g * jax.nn.sigmoid(1.702 * g) * (u + 1.0)).astype(BF16)
        return carry

    lax.fori_loop(0, rows // step, one, 0)
    for c in copies:
        c.wait()


def multiply(order, at, whole, stride):
    per = whole.shape[0] // (SUB * stride)
    acc = None
    for ref, k, wk, r in order:
        lhs = jnp.concatenate([ref[k, at, :], ref[k + 1, at, :]], axis=1)
        rhs = jnp.concatenate(
            [whole[((wk + j) * stride + r) * per + i] for j in range(2) for i in range(per)],
            axis=0,
        )
        part = jnp.dot(lhs, rhs, preferred_element_type=F32)
        acc = part if acc is None else acc + part
    return acc


def down_kernel(ids, *refs, stride, parts):
    five, weights = refs[:5], refs[5 : 5 + parts]
    out, down_out, whole, sems = refs[5 + parts :]
    rows, _ = out.shape
    size = weights[0].shape[1]
    copies = []
    for k, w in enumerate(weights):
        at = part_at(ids[1], k, parts, size)
        copies.append(pltpu.make_async_copy(w, down_out.at[:, at, :], sems.at[k]))
        whole[:, at, :] = w[...]
    for c in copies:
        c.start()
    order = pieces(*five, ids[0], stride)
    step = 128

    def one(i, carry):
        at = pl.ds(pl.multiple_of(i * step, step), step)
        out[at, :] = multiply(order, at, whole, stride).astype(BF16)
        return carry

    lax.fori_loop(0, rows // step, one, 0)
    for c in copies:
        c.wait()


def combine_kernel(comb_hi, comb_lo, rows, mixed):
    dims = (((0,), (0,)), ((), ()))
    acc = lax.dot_general(comb_hi[...], rows[...], dims, preferred_element_type=F32)
    acc = acc + lax.dot_general(comb_lo[...], rows[...], dims, preferred_element_type=F32)
    mixed[...] = acc.astype(BF16)


def exchange(x):
    return lax.all_to_all(x, "tp", split_axis=0, concat_axis=0, tiled=True)


def after(x, *others):
    return lax.optimization_barrier((x, *others))[0]


def gather(block):
    count = lax.axis_size("fs")
    stride = count // SUB
    groups = [[i + stride * j for j in range(SUB)] for i in range(stride)]
    own = lax.all_gather(block, "fs", axis=0, axis_index_groups=groups)

    def shift(x, by):
        return lax.ppermute(x, "fs", [(i, (i + by) % count) for i in range(count)])

    half = SUB // 2
    low, high = own[:half], own[half:]
    return [own, shift(own, 1), shift(own, -1), shift(low, 2), shift(high, -2)]


def other_groups(x):
    count = lax.axis_size("grp")
    return [x] + [
        lax.ppermute(x, "grp", [(i, (i + k) % count) for i in range(count)])
        for k in range(1, count)
    ]


def in_vmem(xs):
    return [pltpu.with_memory_space_constraint(x, pltpu.VMEM) for x in xs]


def body(tokens, route_expert, route_weight, norm_gain, gate_train, up_train, down_train):
    tp_count = lax.axis_size("tp")
    fs_count = lax.axis_size("fs")
    stride = fs_count // SUB
    parts = lax.axis_size("grp")
    tok_rows, width = tokens.shape
    cols = width // fs_count
    slots = EXPERTS * CAP
    my_block = lax.axis_index("fs").astype(jnp.int32)
    my_group = lax.axis_index("grp").astype(jnp.int32)
    ids = jnp.stack([my_block % stride, my_group])

    buffer, comb_hi, comb_lo = pl.pallas_call(
        prep_kernel,
        in_specs=[sm(), vm(), vm(), vm()],
        out_specs=[vm(), vm(), vm()],
        out_shape=[
            jax.ShapeDtypeStruct((slots, cols), BF16),
            jax.ShapeDtypeStruct((slots, tok_rows), BF16),
            jax.ShapeDtypeStruct((slots, tok_rows), BF16),
        ],
        compiler_params=pltpu.CompilerParams(vmem_limit_bytes=16 << 20),
        name="prep",
    )(my_block.reshape(1), tokens, route_expert.T, route_weight.T)
    arrived = exchange(buffer.reshape(EXPERTS, CAP, cols)).reshape(slots, cols)

    size = gate_train.shape[1] // parts

    def share(w):
        return lax.dynamic_slice_in_dim(w, my_group * size, size, 1)

    gain = lax.dynamic_slice_in_dim(norm_gain, my_group * size, size)[None, :, None]
    packed = jnp.concatenate(
        [(share(gate_train) * gain).astype(BF16), (share(up_train) * gain).astype(BF16)], axis=1
    )
    both = exchange(after(packed, arrived))
    down_part = exchange(after(share(down_train).astype(BF16), both))
    served = jax.ShapeDtypeStruct(down_train.shape, BF16)
    hbm = pl.BlockSpec(memory_space=pl.ANY)

    hidden, gate_serve, up_serve = pl.pallas_call(
        functools.partial(gate_up_kernel, stride=stride, parts=parts),
        in_specs=[sm()] + [vm()] * (5 + parts),
        out_specs=[vm(), hbm, hbm],
        out_shape=[jax.ShapeDtypeStruct((slots, both.shape[2]), BF16), served, served],
        scratch_shapes=[
            pltpu.VMEM(served.shape[:2] + (2 * both.shape[2],), BF16),
            pltpu.SemaphoreType.DMA((2 * parts,)),
        ],
        compiler_params=pltpu.CompilerParams(vmem_limit_bytes=16 << 20),
        name="gate_up",
    )(ids, *in_vmem(gather(arrived) + other_groups(both)))
    expert_out, down_serve = pl.pallas_call(
        functools.partial(down_kernel, stride=stride, parts=parts),
        in_specs=[sm()] + [vm()] * (5 + parts),
        out_specs=[vm(), hbm],
        out_shape=[jax.ShapeDtypeStruct((slots, down_train.shape[2]), BF16), served],
        scratch_shapes=[
            pltpu.VMEM(served.shape, BF16),
            pltpu.SemaphoreType.DMA((parts,)),
        ],
        compiler_params=pltpu.CompilerParams(vmem_limit_bytes=16 << 20),
        name="down",
    )(ids, *in_vmem(gather(hidden) + other_groups(down_part)))
    returned = exchange(expert_out.reshape(tp_count, slots // tp_count, -1)).reshape(slots, -1)
    mixed = pl.pallas_call(
        combine_kernel,
        in_specs=[vm()] * 3,
        out_specs=vm(),
        out_shape=jax.ShapeDtypeStruct((tok_rows, returned.shape[1]), BF16),
        compiler_params=pltpu.CompilerParams(vmem_limit_bytes=16 << 20),
        name="combine",
    )(comb_hi, comb_lo, *in_vmem([returned]))

    def whole(w):
        return w.reshape(1, -1, w.shape[-1])

    return (whole(gate_serve), whole(up_serve), whole(down_serve), mixed)


def solution(mesh):
    return jax.shard_map(
        body,
        mesh=mesh,
        in_specs=(
            P(("grp", "tp"), None),
            P(("grp", "tp"), None),
            P(("grp", "tp"), None),
            P("tp"),
            P(None, "tp", "fs"),
            P(None, "tp", "fs"),
            P(None, "tp", "fs"),
        ),
        out_specs=(
            P(("grp", "tp"), None, "fs"),
            P(("grp", "tp"), None, "fs"),
            P(("grp", "tp"), None, "fs"),
            P(("grp", "tp"), "fs"),
        ),
        check_vma=False,
    )
```

```python
import functools

import jax
import jax.numpy as jnp
from jax import lax
from jax.experimental import pallas as pl
from jax.experimental.pallas import tpu as pltpu
from jax.sharding import PartitionSpec as P


EXPERTS = 32
TOP = 4
CAP = 16
SUB = 4
F32 = jnp.float32
BF16 = jnp.bfloat16


def vm():
    return pl.BlockSpec(memory_space=pltpu.VMEM)


def sm():
    return pl.BlockSpec(memory_space=pltpu.SMEM)


def prep_kernel(block, tokens, route_t, weight_t, buffer, comb_hi, comb_lo):
    rows, _ = tokens.shape
    floated = tokens[...].astype(F32)
    inv = lax.rsqrt(jnp.mean(floated * floated, axis=-1, keepdims=True) + 1e-06)
    cols = buffer.shape[1]
    part = tokens[:, pl.ds(pl.multiple_of(block[0] * cols, cols), cols)].astype(F32)
    normed = (part * inv).astype(BF16)
    expert = lax.broadcasted_iota(jnp.int32, (EXPERTS, rows), 0)
    named = jnp.zeros((EXPERTS, rows), F32)
    weight = jnp.zeros((EXPERTS, rows), F32)
    for k in range(TOP):
        hit = route_t[k : k + 1, :] == expert
        named = named + jnp.where(hit, 1.0, 0.0)
        weight = weight + jnp.where(hit, weight_t[k : k + 1, :], 0.0)
    earlier = lax.broadcasted_iota(jnp.int32, (rows, rows), 0) < lax.broadcasted_iota(
        jnp.int32, (rows, rows), 1
    )
    rank = jnp.dot(
        named.astype(BF16),
        jnp.where(earlier, 1.0, 0.0).astype(BF16),
        preferred_element_type=F32,
    )
    rank = jnp.where(named > 0.5, rank, -1.0)
    slot = lax.broadcasted_iota(jnp.int32, (EXPERTS, CAP, rows), 1).astype(F32)
    taken = rank[:, None, :] == slot
    scatter = jnp.where(taken, 1.0, 0.0).reshape(EXPERTS * CAP, rows)
    buffer[...] = jnp.dot(scatter.astype(BF16), normed, preferred_element_type=F32).astype(BF16)
    comb = jnp.where(taken, weight[:, None, :], 0.0).reshape(EXPERTS * CAP, rows)
    high = comb.astype(BF16)
    comb_hi[...] = high
    comb_lo[...] = (comb - high.astype(F32)).astype(BF16)


def pieces(own, first, second, low, high, res, stride):
    half = SUB // 2
    side = (res + 1 + 2 * (1 - res % 2)) % stride
    out = []
    for ref, r in ((own, res), (first, res + 1 - 2 * (res % 2)), (second, side)):
        for k in range(0, SUB, 2):
            out.append((ref, k, k, r))
    for k in range(0, half, 2):
        out.append((low, k, k, (res + 2) % stride))
        out.append((high, k, half + k, (res + 2) % stride))
    return out


def part_at(first, k, parts, size):
    return pl.ds(pl.multiple_of(((first + parts - k) % parts) * size, size), size)


def gate_up_kernel(ids, *refs, stride, parts):
    five, weights = refs[:5], refs[5 : 5 + parts]
    hidden, gate_out, up_out, whole, sems = refs[5 + parts :]
    rows, width = hidden.shape
    size = weights[0].shape[1] // 2
    copies = []
    for k, w in enumerate(weights):
        at = part_at(ids[1], k, parts, size)
        for j, dst in enumerate((gate_out, up_out)):
            src = w.at[:, j * size : (j + 1) * size, :]
            copies.append(pltpu.make_async_copy(src, dst.at[:, at, :], sems.at[2 * k + j]))
            whole[:, at, j * width : (j + 1) * width] = w[:, j * size : (j + 1) * size, :]
    for c in copies:
        c.start()
    order = pieces(*five, ids[0], stride)
    step = 128

    def one(i, carry):
        at = pl.ds(pl.multiple_of(i * step, step), step)
        acc = multiply(order, at, whole, stride)
        g = jnp.minimum(acc[:, :width], 7.0)
        u = jnp.clip(acc[:, width:], -7.0, 7.0)
        hidden[at, :] = (g * jax.nn.sigmoid(1.702 * g) * (u + 1.0)).astype(BF16)
        return carry

    lax.fori_loop(0, rows // step, one, 0)
    for c in copies:
        c.wait()


def multiply(order, at, whole, stride):
    per = whole.shape[0] // (SUB * stride)
    acc = None
    for ref, k, wk, r in order:
        lhs = jnp.concatenate([ref[k, at, :], ref[k + 1, at, :]], axis=1)
        rhs = jnp.concatenate(
            [whole[((wk + j) * stride + r) * per + i] for j in range(2) for i in range(per)],
            axis=0,
        )
        part = jnp.dot(lhs, rhs, preferred_element_type=F32)
        acc = part if acc is None else acc + part
    return acc


def down_kernel(ids, *refs, stride, parts):
    five, weights = refs[:5], refs[5 : 5 + parts]
    out, down_out, whole, sems = refs[5 + parts :]
    rows, _ = out.shape
    size = weights[0].shape[1]
    copies = []
    for k, w in enumerate(weights):
        at = part_at(ids[1], k, parts, size)
        copies.append(pltpu.make_async_copy(w, down_out.at[:, at, :], sems.at[k]))
        whole[:, at, :] = w[...]
    for c in copies:
        c.start()
    order = pieces(*five, ids[0], stride)
    step = 128

    def one(i, carry):
        at = pl.ds(pl.multiple_of(i * step, step), step)
        out[at, :] = multiply(order, at, whole, stride).astype(BF16)
        return carry

    lax.fori_loop(0, rows // step, one, 0)
    for c in copies:
        c.wait()


def combine_kernel(comb_hi, comb_lo, rows, mixed):
    dims = (((0,), (0,)), ((), ()))
    acc = lax.dot_general(comb_hi[...], rows[...], dims, preferred_element_type=F32)
    acc = acc + lax.dot_general(comb_lo[...], rows[...], dims, preferred_element_type=F32)
    mixed[...] = acc.astype(BF16)


def exchange(x):
    return lax.all_to_all(x, "tp", split_axis=0, concat_axis=0, tiled=True)


def after(x, *others):
    return lax.optimization_barrier((x, *others))[0]


def gather(block):
    count = lax.axis_size("fs")
    stride = count // SUB
    groups = [[i + stride * j for j in range(SUB)] for i in range(stride)]
    own = lax.all_gather(block, "fs", axis=0, axis_index_groups=groups)

    def swap(x, partner):
        return lax.ppermute(x, "fs", [(i, partner(i) % count) for i in range(count)])

    half = SUB // 2
    low, high = own[:half], own[half:]
    return [
        own,
        swap(own, lambda i: i ^ 1),
        swap(own, lambda i: i + 1 if i & 1 else i - 1),
        swap(low, lambda i: i ^ 2),
        swap(high, lambda i: i + 2 if i & 2 else i - 2),
    ]


def other_groups(x):
    count = lax.axis_size("grp")
    return [x] + [
        lax.ppermute(x, "grp", [(i, (i + k) % count) for i in range(count)])
        for k in range(1, count)
    ]


def in_vmem(xs):
    return [pltpu.with_memory_space_constraint(x, pltpu.VMEM) for x in xs]


def body(tokens, route_expert, route_weight, norm_gain, gate_train, up_train, down_train):
    tp_count = lax.axis_size("tp")
    fs_count = lax.axis_size("fs")
    stride = fs_count // SUB
    parts = lax.axis_size("grp")
    tok_rows, width = tokens.shape
    cols = width // fs_count
    slots = EXPERTS * CAP
    my_block = lax.axis_index("fs").astype(jnp.int32)
    my_group = lax.axis_index("grp").astype(jnp.int32)
    ids = jnp.stack([my_block % stride, my_group])

    buffer, comb_hi, comb_lo = pl.pallas_call(
        prep_kernel,
        in_specs=[sm(), vm(), vm(), vm()],
        out_specs=[vm(), vm(), vm()],
        out_shape=[
            jax.ShapeDtypeStruct((slots, cols), BF16),
            jax.ShapeDtypeStruct((slots, tok_rows), BF16),
            jax.ShapeDtypeStruct((slots, tok_rows), BF16),
        ],
        name="prep",
    )(my_block.reshape(1), tokens, route_expert.T, route_weight.T)
    arrived = exchange(buffer.reshape(EXPERTS, CAP, cols)).reshape(slots, cols)

    size = gate_train.shape[1] // parts

    def share(w):
        return lax.dynamic_slice_in_dim(w, my_group * size, size, 1)

    gain = lax.dynamic_slice_in_dim(norm_gain, my_group * size, size)[None, :, None]
    packed = jnp.concatenate(
        [(share(gate_train) * gain).astype(BF16), (share(up_train) * gain).astype(BF16)], axis=1
    )
    both = exchange(after(packed, arrived))
    down_part = exchange(after(share(down_train).astype(BF16), both))
    served = jax.ShapeDtypeStruct(down_train.shape, BF16)
    hbm = pl.BlockSpec(memory_space=pl.ANY)

    hidden, gate_serve, up_serve = pl.pallas_call(
        functools.partial(gate_up_kernel, stride=stride, parts=parts),
        in_specs=[sm()] + [vm()] * (5 + parts),
        out_specs=[vm(), hbm, hbm],
        out_shape=[jax.ShapeDtypeStruct((slots, both.shape[2]), BF16), served, served],
        scratch_shapes=[
            pltpu.VMEM(served.shape[:2] + (2 * both.shape[2],), BF16),
            pltpu.SemaphoreType.DMA((2 * parts,)),
        ],
        compiler_params=pltpu.CompilerParams(vmem_limit_bytes=16 << 20),
        name="gate_up",
    )(ids, *in_vmem(gather(arrived) + other_groups(both)))
    expert_out, down_serve = pl.pallas_call(
        functools.partial(down_kernel, stride=stride, parts=parts),
        in_specs=[sm()] + [vm()] * (5 + parts),
        out_specs=[vm(), hbm],
        out_shape=[jax.ShapeDtypeStruct((slots, down_train.shape[2]), BF16), served],
        scratch_shapes=[
            pltpu.VMEM(served.shape, BF16),
            pltpu.SemaphoreType.DMA((parts,)),
        ],
        compiler_params=pltpu.CompilerParams(vmem_limit_bytes=16 << 20),
        name="down",
    )(ids, *in_vmem(gather(hidden) + other_groups(down_part)))
    returned = exchange(expert_out.reshape(tp_count, slots // tp_count, -1)).reshape(slots, -1)
    mixed = pl.pallas_call(
        combine_kernel,
        in_specs=[vm()] * 3,
        out_specs=vm(),
        out_shape=jax.ShapeDtypeStruct((tok_rows, returned.shape[1]), BF16),
        compiler_params=pltpu.CompilerParams(vmem_limit_bytes=16 << 20),
        name="combine",
    )(comb_hi, comb_lo, *in_vmem([returned]))

    def whole(w):
        return w.reshape(1, -1, w.shape[-1])

    return (whole(gate_serve), whole(up_serve), whole(down_serve), mixed)


def solution(mesh):
    return jax.shard_map(
        body,
        mesh=mesh,
        in_specs=(
            P(("grp", "tp"), None),
            P(("grp", "tp"), None),
            P(("grp", "tp"), None),
            P("tp"),
            P(None, "tp", "fs"),
            P(None, "tp", "fs"),
            P(None, "tp", "fs"),
        ),
        out_specs=(
            P(("grp", "tp"), None, "fs"),
            P(("grp", "tp"), None, "fs"),
            P(("grp", "tp"), None, "fs"),
            P(("grp", "tp"), "fs"),
        ),
        check_vma=False,
    )
```

```python
import functools

import jax
import jax.numpy as jnp
from jax import lax
from jax.experimental import pallas as pl
from jax.experimental.pallas import tpu as pltpu
from jax.sharding import PartitionSpec as P


EXPERTS = 32
TOP = 4
CAP = 16
SUB = 4
F32 = jnp.float32
BF16 = jnp.bfloat16


def vm():
    return pl.BlockSpec(memory_space=pltpu.VMEM)


def sm():
    return pl.BlockSpec(memory_space=pltpu.SMEM)


def slots_of(route_t, size, first):
    rows = route_t.shape[1]
    expert = lax.broadcasted_iota(jnp.int32, (EXPERTS, rows), 0)
    named = jnp.zeros((EXPERTS, rows), F32)
    for k in range(TOP):
        named = named + jnp.where(route_t[k : k + 1, :] == expert, 1.0, 0.0)
    earlier = lax.broadcasted_iota(jnp.int32, (rows, rows), 0) < lax.broadcasted_iota(
        jnp.int32, (rows, rows), 1
    )
    rank = jnp.dot(
        named.astype(BF16),
        jnp.where(earlier, 1.0, 0.0).astype(BF16),
        preferred_element_type=F32,
    )
    rank = jnp.where(named > 0.5, rank, -1.0)
    slot = lax.broadcasted_iota(jnp.int32, (EXPERTS, size, rows), 1) + first
    return rank[:, None, :] == slot.astype(F32)


def prep_kernel(where, tokens, route_t, buffer):
    rows, _ = tokens.shape
    cols = buffer.shape[2]
    floated = tokens[...].astype(F32)
    inv = lax.rsqrt(jnp.mean(floated * floated, axis=-1, keepdims=True) + 1e-06)
    for i, (size, first, at) in enumerate(((CAP, 0, 0), (CAP // 2, where[2], CAP))):
        part = tokens[:, pl.ds(pl.multiple_of(where[i] * cols, cols), cols)].astype(F32)
        normed = (part * inv).astype(BF16)
        scatter = jnp.where(slots_of(route_t, size, first), 1.0, 0.0).reshape(EXPERTS * size, rows)
        put = jnp.dot(scatter.astype(BF16), normed, preferred_element_type=F32)
        buffer[:, at : at + size, :] = put.reshape(EXPERTS, size, cols).astype(BF16)


def comb_kernel(route_t, weight_t, comb_hi, comb_lo):
    rows = route_t.shape[1]
    expert = lax.broadcasted_iota(jnp.int32, (EXPERTS, rows), 0)
    weight = jnp.zeros((EXPERTS, rows), F32)
    for k in range(TOP):
        hit = route_t[k : k + 1, :] == expert
        weight = weight + jnp.where(hit, weight_t[k : k + 1, :], 0.0)
    taken = slots_of(route_t, CAP, 0)
    comb = jnp.where(taken, weight[:, None, :], 0.0).reshape(EXPERTS * CAP, rows)
    high = comb.astype(BF16)
    comb_hi[...] = high
    comb_lo[...] = (comb - high.astype(F32)).astype(BF16)


def repack_kernel(got, own, low, high):
    half = SUB // 2
    for k in range(SUB - 1):
        block = got[k, :, :CAP, :]
        own[k] = block
        if k < half:
            low[k] = block
        else:
            high[k - half] = block
    for j in range(2):
        at = slice(j * CAP // 2, (j + 1) * CAP // 2)
        block = got[1 + j, :, CAP:, :]
        own[SUB - 1, :, at, :] = block
        high[SUB - 1 - half, :, at, :] = block


def pieces(own, first, second, low, high, res, stride):
    half = SUB // 2
    side = (res + 1 + 2 * (1 - res % 2)) % stride
    out = []
    for ref, r in ((own, res), (first, res + 1 - 2 * (res % 2)), (second, side)):
        for k in range(0, SUB, 2):
            out.append((ref, k, k, r))
    for k in range(0, half, 2):
        out.append((low, k, k, (res + 2) % stride))
        out.append((high, k, half + k, (res + 2) % stride))
    return out


def part_at(first, k, parts, size):
    return pl.ds(pl.multiple_of(((first + parts - k) % parts) * size, size), size)


def gate_up_kernel(ids, *refs, stride, parts):
    five, weights = refs[:5], refs[5 : 5 + parts]
    hidden, gate_out, up_out, whole, sems = refs[5 + parts :]
    rows, width = hidden.shape
    size = weights[0].shape[1] // 2
    copies = []
    for k, w in enumerate(weights):
        at = part_at(ids[1], k, parts, size)
        for j, dst in enumerate((gate_out, up_out)):
            src = w.at[:, j * size : (j + 1) * size, :]
            copies.append(pltpu.make_async_copy(src, dst.at[:, at, :], sems.at[2 * k + j]))
            whole[:, at, j * width : (j + 1) * width] = w[:, j * size : (j + 1) * size, :]
    for c in copies:
        c.start()
    order = pieces(*five, ids[0], stride)
    step = 128

    def one(i, carry):
        at = pl.ds(pl.multiple_of(i * step, step), step)
        acc = multiply(order, at, whole, stride)
        g = jnp.minimum(acc[:, :width], 7.0)
        u = jnp.clip(acc[:, width:], -7.0, 7.0)
        hidden[at, :] = (g * jax.nn.sigmoid(1.702 * g) * (u + 1.0)).astype(BF16)
        return carry

    lax.fori_loop(0, rows // step, one, 0)
    for c in copies:
        c.wait()


def multiply(order, at, whole, stride):
    per = whole.shape[0] // (SUB * stride)
    acc = None
    for ref, k, wk, r in order:
        lhs = jnp.concatenate([ref[k, at, :], ref[k + 1, at, :]], axis=1)
        rhs = jnp.concatenate(
            [whole[((wk + j) * stride + r) * per + i] for j in range(2) for i in range(per)],
            axis=0,
        )
        part = jnp.dot(lhs, rhs, preferred_element_type=F32)
        acc = part if acc is None else acc + part
    return acc


def down_kernel(ids, *refs, stride, parts):
    five, weights = refs[:5], refs[5 : 5 + parts]
    out, down_out, whole, sems = refs[5 + parts :]
    rows, _ = out.shape
    size = weights[0].shape[1]
    copies = []
    for k, w in enumerate(weights):
        at = part_at(ids[1], k, parts, size)
        copies.append(pltpu.make_async_copy(w, down_out.at[:, at, :], sems.at[k]))
        whole[:, at, :] = w[...]
    for c in copies:
        c.start()
    order = pieces(*five, ids[0], stride)
    step = 128

    def one(i, carry):
        at = pl.ds(pl.multiple_of(i * step, step), step)
        out[at, :] = multiply(order, at, whole, stride).astype(BF16)
        return carry

    lax.fori_loop(0, rows // step, one, 0)
    for c in copies:
        c.wait()


def combine_kernel(comb_hi, comb_lo, rows, mixed):
    dims = (((0,), (0,)), ((), ()))
    acc = lax.dot_general(comb_hi[...], rows[...], dims, preferred_element_type=F32)
    acc = acc + lax.dot_general(comb_lo[...], rows[...], dims, preferred_element_type=F32)
    mixed[...] = acc.astype(BF16)


def exchange(x):
    return lax.all_to_all(x, "tp", split_axis=0, concat_axis=0, tiled=True)


def after(x, *others):
    return lax.optimization_barrier((x, *others))[0]


def strided(x):
    count = lax.axis_size("fs")
    stride = count // SUB
    groups = [[i + stride * j for j in range(SUB)] for i in range(stride)]
    return lax.all_gather(x, "fs", axis=0, axis_index_groups=groups)


def neighbours(own, low, high):
    count = lax.axis_size("fs")

    def swap(x, partner):
        return lax.ppermute(x, "fs", [(i, partner(i) % count) for i in range(count)])

    return [
        own,
        swap(own, lambda i: i ^ 1),
        swap(own, lambda i: i + 1 if i & 1 else i - 1),
        swap(low, lambda i: i ^ 2),
        swap(high, lambda i: i + 2 if i & 2 else i - 2),
    ]


def gather(block):
    own = strided(block)
    half = SUB // 2
    low, high = own[:half], own[half:]
    return neighbours(own, low, high)


def other_groups(x):
    count = lax.axis_size("grp")
    return [x] + [
        lax.ppermute(x, "grp", [(i, (i + k) % count) for i in range(count)])
        for k in range(1, count)
    ]


def in_vmem(xs):
    return [pltpu.with_memory_space_constraint(x, pltpu.VMEM) for x in xs]


def body(tokens, route_expert, route_weight, norm_gain, gate_train, up_train, down_train):
    tp_count = lax.axis_size("tp")
    fs_count = lax.axis_size("fs")
    stride = fs_count // SUB
    parts = lax.axis_size("grp")
    tok_rows, width = tokens.shape
    cols = width // fs_count
    slots = EXPERTS * CAP
    my_block = lax.axis_index("fs").astype(jnp.int32)
    my_group = lax.axis_index("grp").astype(jnp.int32)
    ids = jnp.stack([my_block % stride, my_group])

    place = my_block // stride
    where = jnp.stack(
        [
            my_block,
            my_block % stride + fs_count - stride,
            jnp.where(place == 2, CAP // 2, 0).astype(jnp.int32),
        ]
    )
    route_t = route_expert.T
    sent = jax.ShapeDtypeStruct((EXPERTS, CAP + CAP // 2, cols), BF16)

    def send(where, tokens, route_t):
        buffer = pl.pallas_call(
            prep_kernel,
            in_specs=[sm(), vm(), vm()],
            out_specs=vm(),
            out_shape=sent,
            name="prep",
        )(where, tokens, route_t)
        return exchange(buffer)

    def skip(where, tokens, route_t):
        return jnp.zeros(sent.shape, sent.dtype)

    arrived = lax.cond(place < SUB - 1, send, skip, where, tokens, route_t)
    comb_hi, comb_lo = pl.pallas_call(
        comb_kernel,
        in_specs=[vm(), vm()],
        out_specs=[vm(), vm()],
        out_shape=[jax.ShapeDtypeStruct((slots, tok_rows), BF16)] * 2,
        name="comb",
    )(route_t, route_weight.T)

    size = gate_train.shape[1] // parts

    def share(w):
        return lax.dynamic_slice_in_dim(w, my_group * size, size, 1)

    gain = lax.dynamic_slice_in_dim(norm_gain, my_group * size, size)[None, :, None]
    packed = jnp.concatenate(
        [(share(gate_train) * gain).astype(BF16), (share(up_train) * gain).astype(BF16)], axis=1
    )
    both = exchange(after(packed, arrived))
    down_part = exchange(after(share(down_train).astype(BF16), both))
    served = jax.ShapeDtypeStruct(down_train.shape, BF16)
    hbm = pl.BlockSpec(memory_space=pl.ANY)

    small = pltpu.CompilerParams(vmem_limit_bytes=16 << 20)
    filled = [(k, EXPERTS, CAP, cols) for k in (SUB, SUB // 2, SUB // 2)]
    packs = pl.pallas_call(
        repack_kernel,
        in_specs=[vm()],
        out_specs=[vm()] * 3,
        out_shape=[jax.ShapeDtypeStruct(shape, BF16) for shape in filled],
        compiler_params=small,
        name="repack",
    )(*in_vmem([strided(arrived)]))
    token_blocks = neighbours(*[p.reshape(p.shape[0], slots, cols) for p in packs])

    hidden, gate_serve, up_serve = pl.pallas_call(
        functools.partial(gate_up_kernel, stride=stride, parts=parts),
        in_specs=[sm()] + [vm()] * (5 + parts),
        out_specs=[vm(), hbm, hbm],
        out_shape=[jax.ShapeDtypeStruct((slots, both.shape[2]), BF16), served, served],
        scratch_shapes=[
            pltpu.VMEM(served.shape[:2] + (2 * both.shape[2],), BF16),
            pltpu.SemaphoreType.DMA((2 * parts,)),
        ],
        compiler_params=pltpu.CompilerParams(vmem_limit_bytes=16 << 20),
        name="gate_up",
    )(ids, *in_vmem(token_blocks + other_groups(both)))
    expert_out, down_serve = pl.pallas_call(
        functools.partial(down_kernel, stride=stride, parts=parts),
        in_specs=[sm()] + [vm()] * (5 + parts),
        out_specs=[vm(), hbm],
        out_shape=[jax.ShapeDtypeStruct((slots, down_train.shape[2]), BF16), served],
        scratch_shapes=[
            pltpu.VMEM(served.shape, BF16),
            pltpu.SemaphoreType.DMA((parts,)),
        ],
        compiler_params=pltpu.CompilerParams(vmem_limit_bytes=16 << 20),
        name="down",
    )(ids, *in_vmem(gather(hidden) + other_groups(down_part)))
    returned = exchange(expert_out.reshape(tp_count, slots // tp_count, -1)).reshape(slots, -1)
    mixed = pl.pallas_call(
        combine_kernel,
        in_specs=[vm()] * 3,
        out_specs=vm(),
        out_shape=jax.ShapeDtypeStruct((tok_rows, returned.shape[1]), BF16),
        compiler_params=pltpu.CompilerParams(vmem_limit_bytes=16 << 20),
        name="combine",
    )(comb_hi, comb_lo, *in_vmem([returned]))

    def whole(w):
        return w.reshape(1, -1, w.shape[-1])

    return (whole(gate_serve), whole(up_serve), whole(down_serve), mixed)


def solution(mesh):
    return jax.shard_map(
        body,
        mesh=mesh,
        in_specs=(
            P(("grp", "tp"), None),
            P(("grp", "tp"), None),
            P(("grp", "tp"), None),
            P("tp"),
            P(None, "tp", "fs"),
            P(None, "tp", "fs"),
            P(None, "tp", "fs"),
        ),
        out_specs=(
            P(("grp", "tp"), None, "fs"),
            P(("grp", "tp"), None, "fs"),
            P(("grp", "tp"), None, "fs"),
            P(("grp", "tp"), "fs"),
        ),
        check_vma=False,
    )
```

```python
import functools

import jax
import jax.numpy as jnp
from jax import lax
from jax.experimental import pallas as pl
from jax.experimental.pallas import tpu as pltpu
from jax.sharding import PartitionSpec as P


EXPERTS = 32
TOP = 4
CAP = 16
SUB = 4
F32 = jnp.float32
BF16 = jnp.bfloat16


def vm():
    return pl.BlockSpec(memory_space=pltpu.VMEM)


def sm():
    return pl.BlockSpec(memory_space=pltpu.SMEM)


def slots_of(route_t, size, first):
    rows = route_t.shape[1]
    expert = lax.broadcasted_iota(jnp.int32, (EXPERTS, rows), 0)
    named = jnp.zeros((EXPERTS, rows), F32)
    for k in range(TOP):
        named = named + jnp.where(route_t[k : k + 1, :] == expert, 1.0, 0.0)
    earlier = lax.broadcasted_iota(jnp.int32, (rows, rows), 0) < lax.broadcasted_iota(
        jnp.int32, (rows, rows), 1
    )
    rank = jnp.dot(
        named.astype(BF16),
        jnp.where(earlier, 1.0, 0.0).astype(BF16),
        preferred_element_type=F32,
    )
    rank = jnp.where(named > 0.5, rank, -1.0)
    slot = lax.broadcasted_iota(jnp.int32, (EXPERTS, size, rows), 1) + first
    return rank[:, None, :] == slot.astype(F32)


def prep_kernel(where, tokens, route_t, buffer):
    rows, _ = tokens.shape
    cols = buffer.shape[2]
    floated = tokens[...].astype(F32)
    inv = lax.rsqrt(jnp.mean(floated * floated, axis=-1, keepdims=True) + 1e-06)
    for i, (size, first, at) in enumerate(((CAP, 0, 0), (CAP // 2, where[2], CAP))):
        part = tokens[:, pl.ds(pl.multiple_of(where[i] * cols, cols), cols)].astype(F32)
        normed = (part * inv).astype(BF16)
        scatter = jnp.where(slots_of(route_t, size, first), 1.0, 0.0).reshape(EXPERTS * size, rows)
        put = jnp.dot(scatter.astype(BF16), normed, preferred_element_type=F32)
        buffer[:, at : at + size, :] = put.reshape(EXPERTS, size, cols).astype(BF16)


def comb_kernel(route_t, weight_t, comb_hi, comb_lo):
    rows = route_t.shape[1]
    expert = lax.broadcasted_iota(jnp.int32, (EXPERTS, rows), 0)
    weight = jnp.zeros((EXPERTS, rows), F32)
    for k in range(TOP):
        hit = route_t[k : k + 1, :] == expert
        weight = weight + jnp.where(hit, weight_t[k : k + 1, :], 0.0)
    taken = slots_of(route_t, CAP, 0)
    comb = jnp.where(taken, weight[:, None, :], 0.0).reshape(EXPERTS * CAP, rows)
    high = comb.astype(BF16)
    comb_hi[...] = high
    comb_lo[...] = (comb - high.astype(F32)).astype(BF16)


def repack_kernel(got, own, low, high):
    half = SUB // 2
    for k in range(SUB - 1):
        block = got[k, :, :CAP, :]
        own[k] = block
        if k < half:
            low[k] = block
        else:
            high[k - half] = block
    for j in range(2):
        at = slice(j * CAP // 2, (j + 1) * CAP // 2)
        block = got[1 + j, :, CAP:, :]
        own[SUB - 1, :, at, :] = block
        high[SUB - 1 - half, :, at, :] = block


def pieces(own, first, second, low, high, res, stride):
    half = SUB // 2
    side = (res + 1 + 2 * (1 - res % 2)) % stride
    out = []
    for ref, r in ((own, res), (first, res + 1 - 2 * (res % 2)), (second, side)):
        for k in range(0, SUB, 2):
            out.append((ref, k, k, r))
    for k in range(0, half, 2):
        out.append((low, k, k, (res + 2) % stride))
        out.append((high, k, half + k, (res + 2) % stride))
    return out


def pack_kernel(group, gate, up, down, gain, out):
    size = gain.shape[0]
    out[:, :size, :] = (gate[...] * gain[...]).astype(BF16)
    out[:, size : 2 * size, :] = (up[...] * gain[...]).astype(BF16)
    out[:, 2 * size :, :] = down[...].astype(BF16)


def part_at(first, k, parts, size):
    return pl.ds(pl.multiple_of(((first + parts - k) % parts) * size, size), size)


def gate_up_kernel(ids, *refs, stride, parts):
    five, weights = refs[:5], refs[5 : 5 + parts]
    hidden, gate_out, up_out, whole, sems = refs[5 + parts :]
    rows, width = hidden.shape
    size = weights[0].shape[1] // 3
    copies = []
    for k, w in enumerate(weights):
        at = part_at(ids[1], k, parts, size)
        for j, dst in enumerate((gate_out, up_out)):
            src = w.at[:, j * size : (j + 1) * size, :]
            copies.append(pltpu.make_async_copy(src, dst.at[:, at, :], sems.at[2 * k + j]))
            whole[:, at, j * width : (j + 1) * width] = w[:, j * size : (j + 1) * size, :]
    for c in copies:
        c.start()
    order = pieces(*five, ids[0], stride)
    step = 128

    def one(i, carry):
        at = pl.ds(pl.multiple_of(i * step, step), step)
        acc = multiply(order, at, whole, stride)
        g = jnp.minimum(acc[:, :width], 7.0)
        u = jnp.clip(acc[:, width:], -7.0, 7.0)
        hidden[at, :] = (g * jax.nn.sigmoid(1.702 * g) * (u + 1.0)).astype(BF16)
        return carry

    lax.fori_loop(0, rows // step, one, 0)
    for c in copies:
        c.wait()


def multiply(order, at, whole, stride):
    per = whole.shape[0] // (SUB * stride)
    acc = None
    for ref, k, wk, r in order:
        lhs = jnp.concatenate([ref[k, at, :], ref[k + 1, at, :]], axis=1)
        rhs = jnp.concatenate(
            [whole[((wk + j) * stride + r) * per + i] for j in range(2) for i in range(per)],
            axis=0,
        )
        part = jnp.dot(lhs, rhs, preferred_element_type=F32)
        acc = part if acc is None else acc + part
    return acc


def down_kernel(ids, *refs, stride, parts):
    five, weights = refs[:5], refs[5 : 5 + parts]
    out, down_out, whole, sems = refs[5 + parts :]
    rows, _ = out.shape
    size = weights[0].shape[1] // 3
    copies = []
    for k, w in enumerate(weights):
        at = part_at(ids[1], k, parts, size)
        src = w.at[:, 2 * size :, :]
        copies.append(pltpu.make_async_copy(src, down_out.at[:, at, :], sems.at[k]))
        whole[:, at, :] = w[:, 2 * size :, :]
    for c in copies:
        c.start()
    order = pieces(*five, ids[0], stride)
    step = 128

    def one(i, carry):
        at = pl.ds(pl.multiple_of(i * step, step), step)
        out[at, :] = multiply(order, at, whole, stride).astype(BF16)
        return carry

    lax.fori_loop(0, rows // step, one, 0)
    for c in copies:
        c.wait()


def combine_kernel(comb_hi, comb_lo, rows, mixed):
    dims = (((0,), (0,)), ((), ()))
    acc = lax.dot_general(comb_hi[...], rows[...], dims, preferred_element_type=F32)
    acc = acc + lax.dot_general(comb_lo[...], rows[...], dims, preferred_element_type=F32)
    mixed[...] = acc.astype(BF16)


def exchange(x):
    return lax.all_to_all(x, "tp", split_axis=0, concat_axis=0, tiled=True)


def after(x, *others):
    return lax.optimization_barrier((x, *others))[0]


def strided(x):
    count = lax.axis_size("fs")
    stride = count // SUB
    groups = [[i + stride * j for j in range(SUB)] for i in range(stride)]
    return lax.all_gather(x, "fs", axis=0, axis_index_groups=groups)


def neighbours(own, low, high):
    count = lax.axis_size("fs")

    def swap(x, partner):
        return lax.ppermute(x, "fs", [(i, partner(i) % count) for i in range(count)])

    return [
        own,
        swap(own, lambda i: i ^ 1),
        swap(own, lambda i: i + 1 if i & 1 else i - 1),
        swap(low, lambda i: i ^ 2),
        swap(high, lambda i: i + 2 if i & 2 else i - 2),
    ]


def gather(block):
    own = strided(block)
    half = SUB // 2
    low, high = own[:half], own[half:]
    return neighbours(own, low, high)


def other_groups(x):
    count = lax.axis_size("grp")
    return [x] + [
        lax.ppermute(x, "grp", [(i, (i + k) % count) for i in range(count)])
        for k in range(1, count)
    ]


def in_vmem(xs):
    return [pltpu.with_memory_space_constraint(x, pltpu.VMEM) for x in xs]


def body(tokens, route_expert, route_weight, norm_gain, gate_train, up_train, down_train):
    tp_count = lax.axis_size("tp")
    fs_count = lax.axis_size("fs")
    stride = fs_count // SUB
    parts = lax.axis_size("grp")
    tok_rows, width = tokens.shape
    cols = width // fs_count
    slots = EXPERTS * CAP
    my_block = lax.axis_index("fs").astype(jnp.int32)
    my_group = lax.axis_index("grp").astype(jnp.int32)
    ids = jnp.stack([my_block % stride, my_group])

    place = my_block // stride
    where = jnp.stack(
        [
            my_block,
            my_block % stride + fs_count - stride,
            jnp.where(place == 2, CAP // 2, 0).astype(jnp.int32),
        ]
    )
    route_t = route_expert.T
    sent = jax.ShapeDtypeStruct((EXPERTS, CAP + CAP // 2, cols), BF16)

    def send(where, tokens, route_t):
        buffer = pl.pallas_call(
            prep_kernel,
            in_specs=[sm(), vm(), vm()],
            out_specs=vm(),
            out_shape=sent,
            name="prep",
        )(where, tokens, route_t)
        return exchange(buffer)

    def skip(where, tokens, route_t):
        return jnp.zeros(sent.shape, sent.dtype)

    arrived = lax.cond(place < SUB - 1, send, skip, where, tokens, route_t)
    comb_hi, comb_lo = pl.pallas_call(
        comb_kernel,
        in_specs=[vm(), vm()],
        out_specs=[vm(), vm()],
        out_shape=[jax.ShapeDtypeStruct((slots, tok_rows), BF16)] * 2,
        name="comb",
    )(route_t, route_weight.T)

    size = gate_train.shape[1] // parts

    step = 8
    taken = (step, size, gate_train.shape[2])
    train_spec = pl.BlockSpec(taken, lambda i, group: (i, group[0], 0))
    gain = jnp.broadcast_to(norm_gain[:, None], (norm_gain.shape[0], taken[2]))
    packed = pl.pallas_call(
        pack_kernel,
        grid_spec=pltpu.PrefetchScalarGridSpec(
            num_scalar_prefetch=1,
            grid=(EXPERTS // step,),
            in_specs=[train_spec] * 3 + [pl.BlockSpec(taken[1:], lambda i, group: (group[0], 0))],
            out_specs=pl.BlockSpec((step, 3 * size, taken[2]), lambda i, group: (i, 0, 0)),
        ),
        out_shape=jax.ShapeDtypeStruct((EXPERTS, 3 * size, taken[2]), BF16),
        name="pack",
    )(my_group.reshape(1), gate_train, up_train, down_train, gain)
    weights = in_vmem(other_groups(exchange(after(packed, arrived))))
    served = jax.ShapeDtypeStruct(down_train.shape, BF16)
    hbm = pl.BlockSpec(memory_space=pl.ANY)

    small = pltpu.CompilerParams(vmem_limit_bytes=16 << 20)
    filled = [(k, EXPERTS, CAP, cols) for k in (SUB, SUB // 2, SUB // 2)]
    packs = pl.pallas_call(
        repack_kernel,
        in_specs=[vm()],
        out_specs=[vm()] * 3,
        out_shape=[jax.ShapeDtypeStruct(shape, BF16) for shape in filled],
        compiler_params=small,
        name="repack",
    )(*in_vmem([strided(arrived)]))
    token_blocks = neighbours(*[p.reshape(p.shape[0], slots, cols) for p in packs])

    hidden, gate_serve, up_serve = pl.pallas_call(
        functools.partial(gate_up_kernel, stride=stride, parts=parts),
        in_specs=[sm()] + [vm()] * (5 + parts),
        out_specs=[vm(), hbm, hbm],
        out_shape=[jax.ShapeDtypeStruct((slots, gate_train.shape[2]), BF16), served, served],
        scratch_shapes=[
            pltpu.VMEM(served.shape[:2] + (2 * gate_train.shape[2],), BF16),
            pltpu.SemaphoreType.DMA((2 * parts,)),
        ],
        compiler_params=pltpu.CompilerParams(vmem_limit_bytes=16 << 20),
        name="gate_up",
    )(ids, *in_vmem(token_blocks), *weights)
    expert_out, down_serve = pl.pallas_call(
        functools.partial(down_kernel, stride=stride, parts=parts),
        in_specs=[sm()] + [vm()] * (5 + parts),
        out_specs=[vm(), hbm],
        out_shape=[jax.ShapeDtypeStruct((slots, down_train.shape[2]), BF16), served],
        scratch_shapes=[
            pltpu.VMEM(served.shape, BF16),
            pltpu.SemaphoreType.DMA((parts,)),
        ],
        compiler_params=pltpu.CompilerParams(vmem_limit_bytes=16 << 20),
        name="down",
    )(ids, *in_vmem(gather(hidden)), *weights)
    returned = exchange(expert_out.reshape(tp_count, slots // tp_count, -1)).reshape(slots, -1)
    mixed = pl.pallas_call(
        combine_kernel,
        in_specs=[vm()] * 3,
        out_specs=vm(),
        out_shape=jax.ShapeDtypeStruct((tok_rows, returned.shape[1]), BF16),
        compiler_params=pltpu.CompilerParams(vmem_limit_bytes=16 << 20),
        name="combine",
    )(comb_hi, comb_lo, *in_vmem([returned]))

    def whole(w):
        return w.reshape(1, -1, w.shape[-1])

    return (whole(gate_serve), whole(up_serve), whole(down_serve), mixed)


def solution(mesh):
    return jax.shard_map(
        body,
        mesh=mesh,
        in_specs=(
            P(("grp", "tp"), None),
            P(("grp", "tp"), None),
            P(("grp", "tp"), None),
            P("tp"),
            P(None, "tp", "fs"),
            P(None, "tp", "fs"),
            P(None, "tp", "fs"),
        ),
        out_specs=(
            P(("grp", "tp"), None, "fs"),
            P(("grp", "tp"), None, "fs"),
            P(("grp", "tp"), None, "fs"),
            P(("grp", "tp"), "fs"),
        ),
        check_vma=False,
    )
```

```python
import functools

import jax
import jax.numpy as jnp
from jax import lax
from jax.experimental import pallas as pl
from jax.experimental.pallas import tpu as pltpu
from jax.sharding import PartitionSpec as P


EXPERTS = 32
TOP = 4
CAP = 16
SUB = 4
F32 = jnp.float32
BF16 = jnp.bfloat16


def vm():
    return pl.BlockSpec(memory_space=pltpu.VMEM)


def sm():
    return pl.BlockSpec(memory_space=pltpu.SMEM)


def slots_of(route_t, size, first):
    rows = route_t.shape[1]
    expert = lax.broadcasted_iota(jnp.int32, (EXPERTS, rows), 0)
    named = jnp.zeros((EXPERTS, rows), F32)
    for k in range(TOP):
        named = named + jnp.where(route_t[k : k + 1, :] == expert, 1.0, 0.0)
    earlier = lax.broadcasted_iota(jnp.int32, (rows, rows), 0) < lax.broadcasted_iota(
        jnp.int32, (rows, rows), 1
    )
    rank = jnp.dot(
        named.astype(BF16),
        jnp.where(earlier, 1.0, 0.0).astype(BF16),
        preferred_element_type=F32,
    )
    rank = jnp.where(named > 0.5, rank, -1.0)
    slot = lax.broadcasted_iota(jnp.int32, (EXPERTS, size, rows), 1) + first
    return rank[:, None, :] == slot.astype(F32)


def prep_kernel(where, tokens, route_t, buffer):
    rows, _ = tokens.shape
    cols = buffer.shape[2]
    floated = tokens[...].astype(F32)
    inv = lax.rsqrt(jnp.mean(floated * floated, axis=-1, keepdims=True) + 1e-06)
    for i, (size, first, at) in enumerate(((CAP, 0, 0), (CAP // 2, where[2], CAP))):
        part = tokens[:, pl.ds(pl.multiple_of(where[i] * cols, cols), cols)].astype(F32)
        normed = (part * inv).astype(BF16)
        scatter = jnp.where(slots_of(route_t, size, first), 1.0, 0.0).reshape(EXPERTS * size, rows)
        put = jnp.dot(scatter.astype(BF16), normed, preferred_element_type=F32)
        buffer[:, at : at + size, :] = put.reshape(EXPERTS, size, cols).astype(BF16)


def comb_kernel(route_t, weight_t, comb_hi, comb_lo):
    rows = route_t.shape[1]
    expert = lax.broadcasted_iota(jnp.int32, (EXPERTS, rows), 0)
    weight = jnp.zeros((EXPERTS, rows), F32)
    for k in range(TOP):
        hit = route_t[k : k + 1, :] == expert
        weight = weight + jnp.where(hit, weight_t[k : k + 1, :], 0.0)
    taken = slots_of(route_t, CAP, 0)
    comb = jnp.where(taken, weight[:, None, :], 0.0).reshape(EXPERTS * CAP, rows)
    high = comb.astype(BF16)
    comb_hi[...] = high
    comb_lo[...] = (comb - high.astype(F32)).astype(BF16)


def repack_kernel(got, own, low, high):
    half = SUB // 2
    for k in range(SUB - 1):
        block = got[k, :, :CAP, :]
        own[k] = block
        if k < half:
            low[k] = block
        else:
            high[k - half] = block
    for j in range(2):
        at = slice(j * CAP // 2, (j + 1) * CAP // 2)
        block = got[1 + j, :, CAP:, :]
        own[SUB - 1, :, at, :] = block
        high[SUB - 1 - half, :, at, :] = block


def pieces(own, first, second, low, high, res, stride):
    half = SUB // 2
    side = (res + 1 + 2 * (1 - res % 2)) % stride
    out = []
    for ref, r in ((own, res), (first, res + 1 - 2 * (res % 2)), (second, side)):
        for k in range(0, SUB, 2):
            out.append((ref, k, k, r))
    for k in range(0, half, 2):
        out.append((low, k, k, (res + 2) % stride))
        out.append((high, k, half + k, (res + 2) % stride))
    return out


def pack_kernel(group, gate, up, down, gain, out, column):
    size, width = gate.shape[1:]
    column[...] = jnp.broadcast_to(gain[...], (width, gain.shape[1])).T
    scale = column[pl.ds(pl.multiple_of(group[0] * size, size), size), :]
    out[:, :size, :] = (gate[...] * scale).astype(BF16)
    out[:, size : 2 * size, :] = (up[...] * scale).astype(BF16)
    out[:, 2 * size :, :] = down[...].astype(BF16)


def part_at(first, k, parts, size):
    return pl.ds(pl.multiple_of(((first + parts - k) % parts) * size, size), size)


def gate_up_kernel(ids, *refs, stride, parts):
    five, weights = refs[:5], refs[5 : 5 + parts]
    hidden, gate_out, up_out, whole, sems = refs[5 + parts :]
    rows, width = hidden.shape
    size = weights[0].shape[1] // 2
    copies = []
    for k, w in enumerate(weights):
        at = part_at(ids[1], k, parts, size)
        for j, dst in enumerate((gate_out, up_out)):
            src = w.at[:, j * size : (j + 1) * size, :]
            copies.append(pltpu.make_async_copy(src, dst.at[:, at, :], sems.at[2 * k + j]))
            whole[:, at, j * width : (j + 1) * width] = w[:, j * size : (j + 1) * size, :]
    for c in copies:
        c.start()
    order = pieces(*five, ids[0], stride)
    step = 128

    def one(i, carry):
        at = pl.ds(pl.multiple_of(i * step, step), step)
        acc = multiply(order, at, whole, stride)
        g = jnp.minimum(acc[:, :width], 7.0)
        u = jnp.clip(acc[:, width:], -7.0, 7.0)
        hidden[at, :] = (g * jax.nn.sigmoid(1.702 * g) * (u + 1.0)).astype(BF16)
        return carry

    lax.fori_loop(0, rows // step, one, 0)
    for c in copies:
        c.wait()


def multiply(order, at, whole, stride):
    per = whole.shape[0] // (SUB * stride)
    acc = None
    for ref, k, wk, r in order:
        lhs = jnp.concatenate([ref[k, at, :], ref[k + 1, at, :]], axis=1)
        rhs = jnp.concatenate(
            [whole[((wk + j) * stride + r) * per + i] for j in range(2) for i in range(per)],
            axis=0,
        )
        part = jnp.dot(lhs, rhs, preferred_element_type=F32)
        acc = part if acc is None else acc + part
    return acc


def down_kernel(ids, *refs, stride, parts):
    five, weights = refs[:5], refs[5 : 5 + parts]
    out, down_out, whole, sems = refs[5 + parts :]
    rows, _ = out.shape
    size = weights[0].shape[1]
    copies = []
    for k, w in enumerate(weights):
        at = part_at(ids[1], k, parts, size)
        copies.append(pltpu.make_async_copy(w, down_out.at[:, at, :], sems.at[k]))
        whole[:, at, :] = w[...]
    for c in copies:
        c.start()
    order = pieces(*five, ids[0], stride)
    step = 128

    def one(i, carry):
        at = pl.ds(pl.multiple_of(i * step, step), step)
        out[at, :] = multiply(order, at, whole, stride).astype(BF16)
        return carry

    lax.fori_loop(0, rows // step, one, 0)
    for c in copies:
        c.wait()


def combine_kernel(comb_hi, comb_lo, rows, mixed):
    dims = (((0,), (0,)), ((), ()))
    acc = lax.dot_general(comb_hi[...], rows[...], dims, preferred_element_type=F32)
    acc = acc + lax.dot_general(comb_lo[...], rows[...], dims, preferred_element_type=F32)
    mixed[...] = acc.astype(BF16)


def exchange(x):
    return lax.all_to_all(x, "tp", split_axis=0, concat_axis=0, tiled=True)


def after(x, *others):
    return lax.optimization_barrier((x, *others))[0]


def strided(x):
    count = lax.axis_size("fs")
    stride = count // SUB
    groups = [[i + stride * j for j in range(SUB)] for i in range(stride)]
    return lax.all_gather(x, "fs", axis=0, axis_index_groups=groups)


def neighbours(own, low, high):
    count = lax.axis_size("fs")

    def swap(x, partner):
        return lax.ppermute(x, "fs", [(i, partner(i) % count) for i in range(count)])

    return [
        own,
        swap(own, lambda i: i ^ 1),
        swap(own, lambda i: i + 1 if i & 1 else i - 1),
        swap(low, lambda i: i ^ 2),
        swap(high, lambda i: i + 2 if i & 2 else i - 2),
    ]


def gather(block):
    own = strided(block)
    half = SUB // 2
    low, high = own[:half], own[half:]
    return neighbours(own, low, high)


def other_groups(x):
    count = lax.axis_size("grp")
    return [x] + [
        lax.ppermute(x, "grp", [(i, (i + k) % count) for i in range(count)])
        for k in range(1, count)
    ]


def in_vmem(xs):
    return [pltpu.with_memory_space_constraint(x, pltpu.VMEM) for x in xs]


def body(tokens, route_expert, route_weight, norm_gain, gate_train, up_train, down_train):
    tp_count = lax.axis_size("tp")
    fs_count = lax.axis_size("fs")
    stride = fs_count // SUB
    parts = lax.axis_size("grp")
    tok_rows, width = tokens.shape
    cols = width // fs_count
    slots = EXPERTS * CAP
    my_block = lax.axis_index("fs").astype(jnp.int32)
    my_group = lax.axis_index("grp").astype(jnp.int32)
    ids = jnp.stack([my_block % stride, my_group])

    place = my_block // stride
    where = jnp.stack(
        [
            my_block,
            my_block % stride + fs_count - stride,
            jnp.where(place == 2, CAP // 2, 0).astype(jnp.int32),
        ]
    )
    route_t = route_expert.T
    sent = jax.ShapeDtypeStruct((EXPERTS, CAP + CAP // 2, cols), BF16)

    def send(where, tokens, route_t):
        buffer = pl.pallas_call(
            prep_kernel,
            in_specs=[sm(), vm(), vm()],
            out_specs=vm(),
            out_shape=sent,
            name="prep",
        )(where, tokens, route_t)
        return exchange(buffer)

    def skip(where, tokens, route_t):
        return jnp.zeros(sent.shape, sent.dtype)

    arrived = lax.cond(place < SUB - 1, send, skip, where, tokens, route_t)
    comb_hi, comb_lo = pl.pallas_call(
        comb_kernel,
        in_specs=[vm(), vm()],
        out_specs=[vm(), vm()],
        out_shape=[jax.ShapeDtypeStruct((slots, tok_rows), BF16)] * 2,
        name="comb",
    )(route_t, route_weight.T)

    size = gate_train.shape[1] // parts

    step = 16
    taken = (step, size, gate_train.shape[2])
    train_spec = pl.BlockSpec(taken, lambda i, group: (i, group[0], 0))
    rows = norm_gain.shape[0]
    packed = pl.pallas_call(
        pack_kernel,
        grid_spec=pltpu.PrefetchScalarGridSpec(
            num_scalar_prefetch=1,
            grid=(EXPERTS // step,),
            in_specs=[train_spec] * 3 + [pl.BlockSpec((1, rows), lambda i, group: (0, 0))],
            out_specs=pl.BlockSpec((step, 3 * size, taken[2]), lambda i, group: (i, 0, 0)),
            scratch_shapes=[pltpu.VMEM((rows, taken[2]), F32)],
        ),
        out_shape=jax.ShapeDtypeStruct((EXPERTS, 3 * size, taken[2]), BF16),
        name="pack",
    )(my_group.reshape(1), gate_train, up_train, down_train, norm_gain.reshape(1, rows))
    served_part = exchange(after(packed, arrived))
    both = in_vmem(other_groups(served_part[:, : 2 * size]))
    downs = in_vmem(other_groups(served_part[:, 2 * size :]))
    served = jax.ShapeDtypeStruct(down_train.shape, BF16)
    hbm = pl.BlockSpec(memory_space=pl.ANY)

    small = pltpu.CompilerParams(vmem_limit_bytes=16 << 20)
    filled = [(k, EXPERTS, CAP, cols) for k in (SUB, SUB // 2, SUB // 2)]
    packs = pl.pallas_call(
        repack_kernel,
        in_specs=[vm()],
        out_specs=[vm()] * 3,
        out_shape=[jax.ShapeDtypeStruct(shape, BF16) for shape in filled],
        compiler_params=small,
        name="repack",
    )(*in_vmem([strided(arrived)]))
    token_blocks = neighbours(*[p.reshape(p.shape[0], slots, cols) for p in packs])

    hidden, gate_serve, up_serve = pl.pallas_call(
        functools.partial(gate_up_kernel, stride=stride, parts=parts),
        in_specs=[sm()] + [vm()] * (5 + parts),
        out_specs=[vm(), hbm, hbm],
        out_shape=[jax.ShapeDtypeStruct((slots, gate_train.shape[2]), BF16), served, served],
        scratch_shapes=[
            pltpu.VMEM(served.shape[:2] + (2 * gate_train.shape[2],), BF16),
            pltpu.SemaphoreType.DMA((2 * parts,)),
        ],
        compiler_params=pltpu.CompilerParams(vmem_limit_bytes=16 << 20),
        name="gate_up",
    )(ids, *in_vmem(token_blocks), *both)
    expert_out, down_serve = pl.pallas_call(
        functools.partial(down_kernel, stride=stride, parts=parts),
        in_specs=[sm()] + [vm()] * (5 + parts),
        out_specs=[vm(), hbm],
        out_shape=[jax.ShapeDtypeStruct((slots, down_train.shape[2]), BF16), served],
        scratch_shapes=[
            pltpu.VMEM(served.shape, BF16),
            pltpu.SemaphoreType.DMA((parts,)),
        ],
        compiler_params=pltpu.CompilerParams(vmem_limit_bytes=16 << 20),
        name="down",
    )(ids, *in_vmem(gather(hidden)), *downs)
    returned = exchange(expert_out.reshape(tp_count, slots // tp_count, -1)).reshape(slots, -1)
    mixed = pl.pallas_call(
        combine_kernel,
        in_specs=[vm()] * 3,
        out_specs=vm(),
        out_shape=jax.ShapeDtypeStruct((tok_rows, returned.shape[1]), BF16),
        compiler_params=pltpu.CompilerParams(vmem_limit_bytes=16 << 20),
        name="combine",
    )(comb_hi, comb_lo, *in_vmem([returned]))

    def whole(w):
        return w.reshape(1, -1, w.shape[-1])

    return (whole(gate_serve), whole(up_serve), whole(down_serve), mixed)


def solution(mesh):
    return jax.shard_map(
        body,
        mesh=mesh,
        in_specs=(
            P(("grp", "tp"), None),
            P(("grp", "tp"), None),
            P(("grp", "tp"), None),
            P("tp"),
            P(None, "tp", "fs"),
            P(None, "tp", "fs"),
            P(None, "tp", "fs"),
        ),
        out_specs=(
            P(("grp", "tp"), None, "fs"),
            P(("grp", "tp"), None, "fs"),
            P(("grp", "tp"), None, "fs"),
            P(("grp", "tp"), "fs"),
        ),
        check_vma=False,
    )
```
